256 devices in a mesh: grp: 2 (over y), sp: 32 (over z, core), tp: 4 (over x).
Axes of the slice: x: 4, y: 2, z: 16, core: 2. Of those that a mesh axis runs over, the one named last changes fastest.
The devices are a block of a 4x16x16 slice.
Arguments:
- query_rows: bfloat16 [8192, 1024], P(('grp', 'sp'), 'tp'), parts along dimension 0, may hold values from -64 to 64
- key_rows: bfloat16 [8192, 512], P(('grp', 'sp'), 'tp'), parts along dimension 0, may hold values from -16 to 16
- value_rows: bfloat16 [8192, 512], P(('grp', 'sp'), 'tp'), parts along dimension 0, may hold values from -6 to 6
- sink_logit: float32 [16], P('tp'), may hold values from 3.5 to 7
- out_weight: bfloat16 [1024, 2048], P('tp'), may hold values from -0.1875 to 0.1875
- residual: bfloat16 [8192, 2048], P(('grp', 'sp', 'tp')), parts along dimension 0, may hold values from -6 to 6
- norm_gain: float32 [2048], replicated, may hold values from 0.1 to 1.9
- routes: int32 [8192, 6], P(('grp', 'sp', 'tp')), parts along dimension 0, may hold values from 0 to 127, as said below
- gate_weights: float32 [8192, 6], P(('grp', 'sp', 'tp')), parts along dimension 0, may hold values from 0.1 to 0.8
- expert_gate: bfloat16 [128, 2048, 512], P(('sp', 'tp')), may hold values from -0.125 to 0.125
- expert_up: bfloat16 [128, 2048, 512], P(('sp', 'tp')), may hold values from -0.125 to 0.125
- expert_down: bfloat16 [128, 512, 2048], P(('sp', 'tp')), may hold values from -0.25 to 0.25
- shared_gate: bfloat16 [2048, 512], P(None, 'tp'), may hold values from -0.125 to 0.125
- shared_up: bfloat16 [2048, 512], P(None, 'tp'), may hold values from -0.125 to 0.125
- shared_down: bfloat16 [512, 2048], P('tp'), may hold values from -0.25 to 0.25
Outputs:
- layer_out: bfloat16 [8192, 2048], P(('grp', 'sp', 'tp')), parts along dimension 0
The draws below stay inside these ranges and needn't reach their ends.
There are 2 independent parts, one for each index of `grp`. The reference program is written for one: setup_inputs(seed, part) draws one part's arguments, and reference() takes and returns one part's arrays. A program takes and returns all parts, laid end to end along the dimension named above; an argument that names none is the same for every part. Nothing has to cross between parts.
Inputs may be any that keep to these rules, and one draw needn't show every extreme that they name: `routes`: in each aligned block of 32 rows (the rows of one device) every row names 6 different experts and no expert is named by more than 3 rows; in every draw some expert is named by exactly 3 rows of every block.
All inputs are finite; a program needn't handle non-finite values.
Results may differ from the reference program's by a relative error of at most 0.015.
Values may be sent and summed in bfloat16 or wider, within the bound.
A program may use at most 64 MiB of HBM per device.

```python
import jax
import jax.numpy as jnp
from jax import lax

D = 2048
HEADS = 16
KVH = 8
HEAD = 64
WINDOW = 128
FF = 512
SHARED = 512
TOPK = 6
TOKENS = 4096
ROWS = 32
EXPERTS = 128
CAP = 3
N_TP = 4


def plant_pair(key):
    query_key = jax.random.fold_in(key, 101)
    keys_key = jax.random.fold_in(key, 102)
    queries = jnp.clip(jax.random.normal(query_key, (TOKENS, HEADS * HEAD), jnp.float32), -6.0, 6.0)
    keys_all = jnp.clip(jax.random.normal(keys_key, (TOKENS, KVH * HEAD), jnp.float32), -6.0, 6.0)
    return (jnp.clip(queries, -64.0, 64.0), jnp.clip(keys_all, -16.0, 16.0))


def draw_query_rows(key, part):
    return plant_pair(key)[0].astype(jnp.bfloat16)


def draw_key_rows(key, part):
    return plant_pair(key)[1].astype(jnp.bfloat16)


def draw_residual(key, part):
    base_key = jax.random.fold_in(key, 201)
    row_key = jax.random.fold_in(key, 202)
    col_key = jax.random.fold_in(key, 203)
    base_draw = jnp.clip(jax.random.normal(base_key, (TOKENS, D), jnp.float32), -3.5, 3.5)
    row_scale = jnp.exp(jax.random.uniform(row_key, (TOKENS, 1), jnp.float32, jnp.log(0.4), jnp.log(4.0)))
    col_scale = jnp.exp(jax.random.uniform(col_key, (1, D), jnp.float32, jnp.log(0.4), jnp.log(4.0)))
    return (0.1 * base_draw * row_scale * col_scale).astype(jnp.bfloat16)


def draw_routes(key, part):
    block_count = TOKENS // ROWS
    special = jax.random.randint(jax.random.fold_in(key, 7), (), 0, EXPERTS)
    smallest = (CAP + 1) // 2

    def one_block(block_key):
        size_key, perm_key, row_key = jax.random.split(block_key, 3)
        group_size = jax.random.randint(size_key, (EXPERTS,), smallest, CAP + 1).at[0].set(CAP)
        group_end = jnp.cumsum(group_size)
        slot_index = jnp.arange(ROWS * TOPK, dtype=jnp.int32)
        group_of = jnp.sum((group_end[None, :] <= slot_index[:, None]).astype(jnp.int32), axis=1)
        others = jax.random.permutation(perm_key, EXPERTS - 1).astype(jnp.int32) + 1
        mapping = (jnp.concatenate([jnp.zeros((1,), jnp.int32), others]) + special) % EXPERTS
        chosen = mapping[group_of].reshape(TOPK, ROWS).T
        return chosen[jax.random.permutation(row_key, ROWS)]
    blocks_out = jax.vmap(one_block)(jax.random.split(jax.random.fold_in(key, 9), block_count))
    return blocks_out.reshape(TOKENS, TOPK).astype(jnp.int32)


def shard_levels(stream_key, extent, shards, least, top_value):
    def one(axis_at, shards_of):
        draws = jax.random.uniform(jax.random.fold_in(jax.random.fold_in(stream_key, 6), axis_at), (shards_of,), jnp.float32, least / len(shards), top_value / len(shards))
        return jnp.repeat(jnp.exp(draws), extent[axis_at] // shards_of).reshape((-1,) + (1,) * (len(extent) - axis_at - 1))

    level = one(*shards[0])
    for cut in shards[1:]:
        level = level * one(*cut)
    return level


def noise(own_key, dims, scale, reach, shards=(), held_as=jnp.bfloat16):
    array = jax.random.normal(own_key, dims, jnp.float32) * scale
    if len(shards) > 0:
        array = shard_levels(own_key, dims, shards, -0.22, 0.18) * array
    return jnp.clip(array, min=-reach, max=reach).astype(held_as)


def setup_inputs(seed: int = 0, part: int = 0) -> dict:
    streams_of = jax.random.split(jax.random.key(seed), 16)
    part_keys = jax.random.split(jax.random.fold_in(streams_of[15], part), 16)
    query_rows = draw_query_rows(jax.random.fold_in(jax.random.fold_in(streams_of[15], part), 71), part)
    key_rows = draw_key_rows(jax.random.fold_in(jax.random.fold_in(streams_of[15], part), 71), part)
    value_rows = noise(part_keys[2], (TOKENS, KVH * HEAD), 1.0, 6.0, ((0, 32), (1, 4)))
    sink_logit = jnp.clip(3.5 + 3.5 * jax.random.uniform(streams_of[3], (HEADS,), jnp.float32) ** shard_levels(streams_of[3], (HEADS,), ((0, 4),), -0.2, 0.2), 3.5, 7.0)
    out_weight = noise(streams_of[4], (HEADS * HEAD, D), (HEADS * HEAD) ** -0.5, 0.1875, ((0, 4),))
    residual = draw_residual(jax.random.fold_in(jax.random.fold_in(streams_of[15], part), 71), part)
    norm_gain = jnp.clip(1.0 + 0.18 * jax.random.normal(streams_of[6], (D,), jnp.float32), 0.1, 1.9)
    routes = draw_routes(jax.random.fold_in(jax.random.fold_in(streams_of[15], part), 71), part)
    gate_weights = jnp.clip(0.1 + 0.7 * jax.random.uniform(part_keys[8], (TOKENS, TOPK), jnp.float32) ** shard_levels(part_keys[8], (TOKENS, TOPK), ((0, 128),), -0.2, 0.2), 0.1, 0.8)
    expert_gate = noise(streams_of[9], (EXPERTS, D, FF), D ** -0.5, 0.125, ((0, 128),))
    expert_up = noise(streams_of[10], (EXPERTS, D, FF), D ** -0.5, 0.125, ((0, 128),))
    expert_down = noise(streams_of[11], (EXPERTS, FF, D), FF ** -0.5, 0.25, ((0, 128),))
    shared_gate = noise(streams_of[12], (D, SHARED), D ** -0.5, 0.125, ((1, 4),))
    shared_up = noise(streams_of[13], (D, SHARED), D ** -0.5, 0.125, ((1, 4),))
    shared_down = noise(streams_of[14], (SHARED, D), SHARED ** -0.5, 0.25, ((0, 4),))
    return {"query_rows": query_rows, "key_rows": key_rows, "value_rows": value_rows, "sink_logit": sink_logit, "out_weight": out_weight, "residual": residual, "norm_gain": norm_gain, "routes": routes, "gate_weights": gate_weights, "expert_gate": expert_gate, "expert_up": expert_up, "expert_down": expert_down, "shared_gate": shared_gate, "shared_up": shared_up, "shared_down": shared_down}


norm_eps = 1e-06

def band_view(tensor, blocks):
    shaped = tensor.reshape(blocks, WINDOW, tensor.shape[1], tensor.shape[2])
    padded = jnp.pad(shaped, ((1, 1), (0, 0), (0, 0), (0, 0)))
    return jnp.concatenate([padded[:-2], padded[1:-1], padded[2:]], axis=1)

def attention(query_rows, key_rows, value_rows, sink_logit):
    length = query_rows.shape[0]
    blocks = length // WINDOW
    groups = HEADS // KVH
    queries = query_rows.astype(jnp.float32).reshape(blocks, WINDOW, KVH, groups, HEAD)
    keyband = band_view(key_rows.astype(jnp.float32).reshape(length, KVH, HEAD), blocks)
    valband = band_view(value_rows.astype(jnp.float32).reshape(length, KVH, HEAD), blocks)
    block_ids = jnp.arange(blocks, dtype=jnp.int32)[:, None, None]
    query_pos = block_ids * WINDOW + jnp.arange(WINDOW, dtype=jnp.int32)[None, :, None]
    key_pos = (block_ids - 1) * WINDOW + jnp.arange(3 * WINDOW, dtype=jnp.int32)[None, None, :]
    in_window = (jnp.abs(key_pos - query_pos) <= WINDOW) & (key_pos >= 0) & (key_pos < length)

    def one_head(head_index):
        query_part = queries[:, :, head_index]
        key_part = keyband[:, :, head_index]
        value_part = valband[:, :, head_index]
        scores = jnp.einsum('nqgd,nkd->ngqk', query_part, key_part) * HEAD ** (-0.5)
        scores = jnp.where(in_window[:, None], scores, -jnp.inf)
        sink_part = lax.dynamic_slice_in_dim(sink_logit, head_index * groups, groups).reshape(1, groups, 1, 1)
        row_max = jnp.maximum(sink_part, lax.optimization_barrier(jnp.max(scores, axis=-1, keepdims=True)))
        shifted = jnp.exp(scores - row_max)
        denominator = jnp.exp(sink_part - row_max) + lax.optimization_barrier(jnp.sum(shifted, axis=-1, keepdims=True))
        weights = lax.optimization_barrier((shifted / denominator).astype(jnp.bfloat16))
        weighted = jnp.einsum('ngqk,nkd->nqgd', weights.astype(jnp.float32), value_part)
        return weighted.astype(jnp.bfloat16)
    heads_out = lax.map(one_head, jnp.arange(KVH, dtype=jnp.int32))
    return jnp.transpose(heads_out, (1, 2, 0, 3, 4)).reshape(length, HEADS * HEAD)

def routed_experts(normed, routes, gate_weights, expert_gate, expert_up, expert_down):
    tokens = normed.shape[0]
    model_width = normed.shape[1]
    copies = tokens * TOPK
    block_rows = 64
    flat_expert = routes.reshape(-1).astype(jnp.int32)
    order_index = jnp.argsort(flat_expert, stable=True).astype(jnp.int32)
    sorted_expert = flat_expert[order_index]
    counts = jax.ops.segment_sum(jnp.ones((copies,), jnp.int32), flat_expert, num_segments=EXPERTS)
    padded_counts = (counts + block_rows - 1) // block_rows * block_rows
    padded_end = jnp.cumsum(padded_counts).astype(jnp.int32)
    padded_start = padded_end - padded_counts
    group_start = (jnp.cumsum(counts) - counts).astype(jnp.int32)
    target = padded_start[sorted_expert] + jnp.arange(copies, dtype=jnp.int32) - group_start[sorted_expert]
    block_count = (copies + EXPERTS * (block_rows - 1) + block_rows - 1) // block_rows
    slot_copy = jnp.full((block_count * block_rows,), copies, jnp.int32).at[target].set(order_index)
    block_first = jnp.arange(block_count, dtype=jnp.int32) * block_rows
    block_expert = jnp.minimum(jnp.searchsorted(padded_end, block_first, side='right'), EXPERTS - 1).astype(jnp.int32)
    copy_token = jnp.concatenate([jnp.arange(copies, dtype=jnp.int32) // TOPK, jnp.full((1,), tokens, jnp.int32)])
    padded_rows = jnp.concatenate([normed, jnp.zeros((1, model_width), normed.dtype)], axis=0)

    def run_block(inputs):
        slot_ids, expert_id = inputs
        block_in = padded_rows[copy_token[slot_ids]]
        gate_part = jnp.dot(block_in, expert_gate[expert_id], preferred_element_type=jnp.float32)
        up_part = jnp.dot(block_in, expert_up[expert_id], preferred_element_type=jnp.float32)
        hidden = (jax.nn.silu(gate_part) * up_part).astype(jnp.bfloat16)
        return jnp.dot(hidden, expert_down[expert_id], preferred_element_type=jnp.float32).astype(jnp.bfloat16)
    outputs = lax.map(run_block, (slot_copy.reshape(block_count, block_rows), block_expert))
    per_copy = jnp.zeros((copies + 1, model_width), jnp.bfloat16).at[slot_copy].set(outputs.reshape(-1, model_width))
    per_copy = lax.optimization_barrier(per_copy[:copies].reshape(tokens, TOPK, model_width))
    return lax.optimization_barrier(jnp.sum(gate_weights[:, :, None] * per_copy.astype(jnp.float32), axis=1))

def shared_expert(normed, shared_gate, shared_up, shared_down):
    gate_part = jnp.dot(normed, shared_gate, preferred_element_type=jnp.float32)
    up_part = jnp.dot(normed, shared_up, preferred_element_type=jnp.float32)
    hidden = (jax.nn.silu(gate_part) * up_part).astype(jnp.bfloat16)
    unit_count = SHARED // N_TP
    totals = jnp.zeros((normed.shape[0], shared_down.shape[1]), jnp.float32)
    for group_index in range(N_TP):
        lower_unit = group_index * unit_count
        partial_sum = jnp.dot(hidden[:, lower_unit:lower_unit + unit_count], shared_down[lower_unit:lower_unit + unit_count], preferred_element_type=jnp.float32)
        totals = totals + lax.optimization_barrier(partial_sum.astype(jnp.bfloat16)).astype(jnp.float32)
    return totals

def reference(query_rows, key_rows, value_rows, sink_logit, out_weight, residual, norm_gain, routes, gate_weights, expert_gate, expert_up, expert_down, shared_gate, shared_up, shared_down):
    attended = attention(query_rows, key_rows, value_rows, sink_logit)
    projected = jnp.dot(attended, out_weight, preferred_element_type=jnp.float32)
    stream = residual.astype(jnp.float32) + projected
    normed = (stream * lax.rsqrt(lax.optimization_barrier(jnp.mean(stream * stream, axis=-1, keepdims=True)) + norm_eps) * norm_gain).astype(jnp.bfloat16)
    routed = routed_experts(normed, routes, gate_weights, expert_gate, expert_up, expert_down)
    shared = shared_expert(normed, shared_gate, shared_up, shared_down)
    return (stream + routed + shared).astype(jnp.bfloat16)
```

```python
import functools

import jax
import jax.numpy as jnp
from jax import lax
from jax.experimental import pallas as pl
from jax.experimental.pallas import tpu as pltpu
from jax.sharding import PartitionSpec as P

HEAD = 64
WINDOW = 128
TOPK = 6
CAP = 3
NCH = 4
PER = 5
NORM_EPS = 1e-06
MESH = pl.DeviceIdType.MESH
F32 = jnp.float32
BF16 = jnp.bfloat16


def iota(shape, dim):
    return lax.broadcasted_iota(jnp.int32, shape, dim)


def dot(a, b):
    return jnp.dot(a, b, preferred_element_type=F32)


def silu(v):
    return v / (1.0 + jnp.exp(-v))


def kernel(
    nz,
    nx,
    q_hbm,
    k_hbm,
    v_hbm,
    sink_ref,
    ow_hbm,
    res_hbm,
    gain_ref,
    routes_ref,
    gw_ref,
    eg_hbm,
    eu_hbm,
    ed_hbm,
    sg_hbm,
    su_hbm,
    sd_hbm,
    out_ref,
    qb,
    kv,
    ow,
    res,
    eg,
    eu,
    ed,
    wsh,
    sd,
    att,
    pbuf,
    precv,
    stream,
    slab,
    shp,
    shr,
    ag,
    meta,
    sel,
    com,
    sb,
    rb,
    eo,
    cb,
    part,
    own,
    rsr,
    rss,
    lsem,
    hsend,
    hrecv,
    psend,
    pecv,
    nsend,
    nrecv,
    ssend,
    srecv,
    agsend,
    agrecv,
    msend,
    mrecv,
    dsend,
    drecv,
    csend,
    crecv,
    rsend,
    rrecv,
):
    rows, width = res.shape
    cw = width // NCH
    half = nz // 2
    plane = 2 * nx
    groups = (nz - 1) // PER
    group_rows = PER * CAP + 1
    order = [0]
    for k in range(1, half):
        order += [k, -k]
    order.append(half)
    slot = {d: i for i, d in enumerate(order)}
    slot[-half] = slot[half]

    sp = lax.axis_index("sp")
    x = lax.axis_index("tp")
    nsp = 2 * nz
    z = sp // 2
    c = sp % 2
    zs = ((z + 1) % nz, (z + nz - 1) % nz)

    def at(z_, c_, x_):
        return {"sp": z_ * 2 + c_, "tp": x_}

    def mate(q):
        dc, dx = q // nx, q % nx
        return (c if dc == 0 else 1 - c), (x + dx) % nx

    def back(q):
        dc, dx = q // nx, q % nx
        return dc * nx + (nx - dx) % nx

    sent = []

    def send(src, dst, ss, rs, device):
        copy = pltpu.make_async_remote_copy(
            src_ref=src,
            dst_ref=dst,
            send_sem=ss,
            recv_sem=rs,
            device_id=device,
            device_id_type=MESH,
        )
        copy.start()
        sent.append(copy)

    me = at(z, c, x)

    def arrived(dst, rs):
        pltpu.make_async_remote_copy(
            src_ref=dst,
            dst_ref=dst,
            send_sem=rs,
            recv_sem=rs,
            device_id=me,
            device_id_type=MESH,
        ).wait_recv()

    barrier = pltpu.get_barrier_semaphore()
    cross = at((z + nz + 2 * c - 1) % nz, 1 - c, x)
    friends = [cross, at(zs[0], c, x), at(zs[1], c, x)]
    for q in range(1, plane):
        cq, xq = mate(q)
        friends.append(at(z, cq, xq))
    for friend in friends:
        pl.semaphore_signal(barrier, inc=1, device_id=friend, device_id_type=MESH)

    loads = []

    def load(src, dst):
        copy = pltpu.make_async_copy(src, dst, lsem.at[len(loads)])
        copy.start()
        loads.append(copy)
        return copy

    span = kv.shape[1] // 3
    load_k = load(k_hbm, kv.at[0, span : 2 * span])
    load_v = load(v_hbm, kv.at[1, span : 2 * span])
    load_q = load(q_hbm, qb)
    load_ow = load(ow_hbm, ow)
    load_res = load(res_hbm, res)
    unit = sg_hbm.shape[1]
    load_sg = load(sg_hbm, wsh.at[:, 0:unit])
    load_su = load(su_hbm, wsh.at[:, unit : 2 * unit])
    load_sd = load(sd_hbm, sd)
    load_eg = load(eg_hbm.at[0], eg)
    load_eu = load(eu_hbm.at[0], eu)
    load_ed = load(ed_hbm.at[0], ed)

    lane = iota((rows, 128), 1)
    ids = routes_ref[...]
    gates = gw_ref[...]
    hot = jnp.zeros((rows, 128), F32)
    for k in range(TOPK):
        hot = hot + jnp.where(lane == ids[:, k : k + 1], 1.0, 0.0)
    below = jnp.where(iota((rows, rows), 0) > iota((rows, rows), 1), 1.0, 0.0)
    before = dot(below.astype(BF16), hot.astype(BF16))
    e_cols = jnp.full((rows, 128), -1.0, F32)
    r_cols = jnp.zeros((rows, 128), F32)
    g_cols = jnp.zeros((rows, 128), F32)
    for k in range(TOPK):
        e_k = ids[:, k : k + 1]
        rank = jnp.sum(jnp.where(lane == e_k, before, 0.0), axis=1, keepdims=True)
        here = lane == k
        e_cols = jnp.where(here, e_k.astype(F32), e_cols)
        r_cols = jnp.where(here, rank, r_cols)
        g_cols = jnp.where(here, gates[:, k : k + 1], g_cols)
    spread = jnp.where((lane & (rows - 1)) == iota((rows, 128), 0), 1.0, 0.0).astype(BF16)

    def on_lanes(cols):
        return dot(cols.T.astype(BF16), spread)[0:8]

    g_high = g_cols.astype(BF16).astype(F32)
    meta[0, 0:8, :] = 4.0 * on_lanes(e_cols) + on_lanes(r_cols)
    meta[0, 8:16, :] = on_lanes(g_high) + on_lanes(g_cols - g_high)

    load_k.wait()
    load_v.wait()
    pl.semaphore_wait(barrier, len(friends))

    mine = kv.at[:, span : 2 * span, :]
    nxt = {"sp": (sp + 1) % nsp, "tp": x}
    prv = {"sp": (sp + nsp - 1) % nsp, "tp": x}
    send(mine, kv.at[:, 0:span, :], hsend.at[0], hrecv.at[0], nxt)
    send(mine, kv.at[:, 2 * span : 3 * span, :], hsend.at[1], hrecv.at[1], prv)

    load_q.wait()
    lane_q = iota((span, 128), 1)
    low = lane_q < HEAD
    heads = []
    for h in range(2 * (qb.shape[1] // 128)):
        pair = qb[:, (h // 2) * 128 : (h // 2) * 128 + 128].astype(F32)
        if h % 2 != h // 2:
            pair = pltpu.roll(pair, HEAD, 1)
        keep = low if h // 2 == 0 else jnp.logical_not(low)
        heads.append(jnp.where(keep, pair, 0.0).astype(BF16))

    row_i = iota((span, 3 * span), 0)
    col_i = iota((span, 3 * span), 1)
    pos = sp * span - span + col_i
    open_ = (col_i >= row_i) & (col_i <= row_i + 2 * WINDOW) & (pos >= 0) & (pos < nsp * span)
    arrived(kv.at[:, 0:span, :], hrecv.at[0])
    arrived(kv.at[:, 2 * span : 3 * span, :], hrecv.at[1])
    keys = kv[0]
    values = kv[1]
    results = []
    for h, query in enumerate(heads):
        scores = lax.dot_general(
            query, keys, (((1,), (1,)), ((), ())), preferred_element_type=F32
        ) * (HEAD**-0.5)
        scores = jnp.where(open_, scores, -jnp.inf)
        sink = sink_ref[h]
        row_max = jnp.maximum(jnp.max(scores, axis=-1, keepdims=True), sink)
        shifted = jnp.exp(scores - row_max)
        denominator = jnp.exp(sink - row_max) + jnp.sum(shifted, axis=-1, keepdims=True)
        weights = (shifted / denominator).astype(BF16)
        got = dot(weights, values)
        if h % 2 != h // 2:
            got = pltpu.roll(got, HEAD, 1)
        results.append(got)
    for pair in range(len(heads) // 2):
        att[:, pair * 128 : pair * 128 + 128] = jnp.where(
            low, results[2 * pair], results[2 * pair + 1]
        ).astype(BF16)

    load_ow.wait()
    attended = att[...]
    for ch in range(NCH):
        cols = slice(ch * cw, (ch + 1) * cw)
        pbuf[:, cols] = dot(attended, ow[:, cols]).astype(BF16)
    for dx in (2, 1, 3):
        xq = (x + dx) % nx
        there = (nx - dx) % nx
        begin = pl.multiple_of(xq * rows, rows)
        send(
            pbuf.at[pl.ds(begin, rows), :],
            precv.at[there],
            psend.at[dx],
            pecv.at[there],
            at(z, c, xq),
        )
    load_res.wait()
    total = res[...].astype(F32) + pbuf[pl.ds(pl.multiple_of(x * rows, rows), rows), :].astype(F32)
    for dx in range(1, nx):
        arrived(precv.at[dx], pecv.at[dx])
    for dx in range(1, nx):
        total = total + precv[dx].astype(F32)
    stream[...] = total
    scale = lax.rsqrt(jnp.mean(total * total, axis=-1, keepdims=True) + NORM_EPS)
    normed = (total * scale * gain_ref[...]).astype(BF16)
    slab[0:rows, :] = normed
    for ch in range(NCH):
        ag[ch, 0:rows, :] = normed[:, ch * cw : (ch + 1) * cw]

    def carries(direction, step, ch):
        return step < half or (step == half and (ch < NCH // 2) == (direction == 0))

    def source(direction, step):
        return slot[-step if direction == 0 else step]

    def block(ch, s):
        return ag.at[ch, s * rows : (s + 1) * rows, :]

    def forward(step, ch, direction):
        if not carries(direction, step, ch):
            return
        a, b = source(direction, step - 1), source(direction, step)
        send(
            block(ch, a),
            block(ch, b),
            agsend.at[direction, step - 1, ch],
            agrecv.at[b, ch],
            at(zs[direction], c, x),
        )

    def forward_meta(step, direction):
        if step == half and direction == 1:
            return
        a, b = source(direction, step - 1), source(direction, step)
        send(
            meta.at[a],
            meta.at[b],
            msend.at[direction, step - 1],
            mrecv.at[b],
            at(zs[direction], c, x),
        )

    def gather_step(step):
        for ch in range(NCH):
            for direction in range(2):
                if carries(direction, step, ch):
                    s = source(direction, step)
                    arrived(block(ch, s), agrecv.at[s, ch])
                    if step < half:
                        forward(step + 1, ch, direction)
        for direction in range(2):
            if not (step == half and direction == 1):
                s = source(direction, step)
                arrived(meta.at[s], mrecv.at[s])
                if step < half:
                    forward_meta(step + 1, direction)

    for ch in range(NCH):
        for direction in range(2):
            forward(1, ch, direction)
    for direction in range(2):
        forward_meta(1, direction)
    for dx in (2, 1, 3):
        there = (nx - dx) % nx
        send(
            slab.at[0:rows, :],
            slab.at[there * rows : (there + 1) * rows, :],
            nsend.at[dx],
            nrecv.at[there],
            at(z, c, (x + dx) % nx),
        )

    def shared_expert():
        for dx in range(1, nx):
            arrived(slab.at[dx * rows : (dx + 1) * rows, :], nrecv.at[dx])
        load_sg.wait()
        load_su.wait()
        load_sd.wait()
        both = dot(slab[...], wsh[...])
        hidden = (silu(both[:, 0:unit]) * both[:, unit : 2 * unit]).astype(BF16)
        for ch in range(NCH):
            cols = slice(ch * cw, (ch + 1) * cw)
            shp[:, cols] = dot(hidden, sd[:, cols]).astype(BF16)
        for dx in (2, 1, 3):
            there = (nx - dx) % nx
            send(
                shp.at[dx * rows : (dx + 1) * rows, :],
                shr.at[there],
                ssend.at[dx],
                srecv.at[there],
                at(z, c, (x + dx) % nx),
            )

    def build(g):
        lane8 = iota((8, 128), 1)
        seg8 = lane8 // rows
        codes, gws = [], []
        for v in range(2):
            code = jnp.full((8, 128), -4.0, F32)
            gate = jnp.zeros((8, 128), F32)
            for i in range(4):
                p = 4 * v + i
                if p > PER:
                    continue
                s = 0 if p == 0 else PER * g + p
                code = jnp.where(seg8 == i, meta[s, 0:8, :], code)
                gate = jnp.where(seg8 == i, meta[s, 8:16, :], gate)
            codes.append(code)
            gws.append(gate)
        rr = iota((group_rows, 128), 0)
        bi = (rr * 11) >> 5
        last = rr == group_rows - 1
        pos_r = jnp.where(last, 0, 1 + bi)
        rank_r = jnp.where(last, g, rr - 3 * bi)
        seg = iota((group_rows, 128), 1) // rows
        turned = []
        for q in range(plane):
            cq, xq = mate(q)
            expert = plane * z + nx * cq + xq
            want = (rank_r + 4 * expert).astype(F32)
            lines = []
            for v in range(2):
                placed = pos_r == seg + 4 * v
                one = jnp.zeros((group_rows, 128), F32)
                weight = jnp.zeros((group_rows, 128), F32)
                for k in range(TOPK):
                    match = (codes[v][k : k + 1, :] == want) & placed
                    one = jnp.where(match, 1.0, one)
                    weight = jnp.where(match, gws[v][k : k + 1, :], weight)
                sel[g, q * group_rows : (q + 1) * group_rows, v * 128 : (v + 1) * 128] = one.astype(
                    BF16
                )
                lines.append(weight)
            turned.append(lines)
        for v in range(2):
            column = jnp.concatenate([turned[q][v] for q in range(plane)], axis=0)
            com[g, v * 128 : (v + 1) * 128, :] = column.T.astype(BF16)

    def dispatch(g):
        build(g)
        choose = sel[g]
        for ch in range(NCH):
            cols = slice(ch * cw, (ch + 1) * cw)
            first = ag[ch, 0:rows, :]
            begin = (1 + PER * g) * rows
            stack = jnp.concatenate(
                [first, ag[ch, begin : begin + PER * rows, :], first, first], axis=0
            )
            picked = dot(choose, stack).astype(BF16)
            rb[g, 0:group_rows, cols] = picked[0:group_rows]
            sb[g, group_rows:, cols] = picked[group_rows:]
        for q in far:
            cq, xq = mate(q)
            b = back(q)
            send(
                sb.at[g, q * group_rows : (q + 1) * group_rows, :],
                rb.at[g, b * group_rows : (b + 1) * group_rows, :],
                dsend.at[g, q],
                drecv.at[g, b],
                at(z, cq, xq),
            )

    far = [2, nx + 2, 1, nx + 1, 3, nx + 3, nx]

    def experts(g):
        for q in range(1, plane):
            arrived(rb.at[g, q * group_rows : (q + 1) * group_rows, :], drecv.at[g, q])
        taken = rb[g]
        hidden = (silu(dot(taken, eg[...])) * dot(taken, eu[...])).astype(BF16)
        for ch in range(NCH):
            cols = slice(ch * cw, (ch + 1) * cw)
            made = dot(hidden, ed[:, cols]).astype(BF16)
            cb[g, 0:group_rows, cols] = made[0:group_rows]
            eo[g, group_rows:, cols] = made[group_rows:]
        for q in far:
            cq, xq = mate(q)
            b = back(q)
            send(
                eo.at[g, q * group_rows : (q + 1) * group_rows, :],
                cb.at[g, b * group_rows : (b + 1) * group_rows, :],
                csend.at[g, q],
                crecv.at[g, b],
                at(z, cq, xq),
            )

    def combine(g):
        for q in range(1, plane):
            arrived(cb.at[g, q * group_rows : (q + 1) * group_rows, :], crecv.at[g, q])
        used = (PER + 1) * rows
        mix = com[g, 0:used, :]
        for ch in range(NCH):
            cols = slice(ch * cw, (ch + 1) * cw)
            summed = dot(mix, cb[g, :, cols])
            if g == 0:
                own[:, cols] = summed[0:rows]
            else:
                own[:, cols] = own[:, cols] + summed[0:rows]
            part[g * PER * rows : (g + 1) * PER * rows, cols] = summed[rows:used]

    gather_step(1)
    shared_expert()
    gather_step(2)
    gather_step(3)
    dispatch(0)
    gather_step(4)
    gather_step(5)
    dispatch(1)
    gather_step(6)
    load_eg.wait()
    load_eu.wait()
    load_ed.wait()
    experts(0)
    gather_step(7)
    gather_step(8)
    dispatch(2)
    experts(1)
    combine(0)
    experts(2)
    combine(1)
    combine(2)

    def brings(direction, step, ch):
        return step > 1 or (ch < NCH // 2) == (direction == 0)

    for step in range(1, half + 1):
        distance = half + 1 - step
        for ch in range(NCH):
            cols = slice(ch * cw, (ch + 1) * cw)
            for direction in range(2):
                if not brings(direction, step, ch):
                    continue
                s = slot[distance if direction == 0 else -distance]
                value = part[(s - 1) * rows : s * rows, cols]
                if step > 1 and brings(direction, step - 1, ch):
                    arrived(rsr.at[direction, step - 2, ch], rrecv.at[direction, step - 2, ch])
                    value = value + rsr[direction, step - 2, ch].astype(F32)
                rss[direction, step - 1, ch] = value.astype(BF16)
                send(
                    rss.at[direction, step - 1, ch],
                    rsr.at[direction, step - 1, ch],
                    rsend.at[direction, step - 1, ch],
                    rrecv.at[direction, step - 1, ch],
                    at(zs[direction], c, x),
                )

    base = stream[...] + shp[0:rows, :].astype(F32)
    for dx in range(1, nx):
        arrived(shr.at[dx], srecv.at[dx])
        base = base + shr[dx].astype(F32)
    stream[...] = base + own[...]
    for ch in range(NCH):
        cols = slice(ch * cw, (ch + 1) * cw)
        value = stream[:, cols]
        for direction in range(2):
            arrived(rsr.at[direction, half - 1, ch], rrecv.at[direction, half - 1, ch])
            value = value + rsr[direction, half - 1, ch].astype(F32)
        out_ref[:, cols] = value.astype(BF16)
    for copy in sent:
        copy.wait_send()


def body(nz, nx, *args):
    (
        query_rows,
        key_rows,
        value_rows,
        sink_logit,
        out_weight,
        residual,
        norm_gain,
        routes,
        gate_weights,
        expert_gate,
        expert_up,
        expert_down,
        shared_gate,
        shared_up,
        shared_down,
    ) = args
    rows, width = residual.shape
    span = query_rows.shape[0]
    half = nz // 2
    plane = 2 * nx
    groups = (nz - 1) // PER
    group_rows = PER * CAP + 1
    cw = width // NCH
    ff = expert_gate.shape[2]
    unit = shared_gate.shape[1]
    dma = pltpu.SemaphoreType.DMA
    vm = pltpu.VMEM
    scratch = [
        vm((span, query_rows.shape[1]), BF16),
        vm((2, 3 * span, key_rows.shape[1]), BF16),
        vm(out_weight.shape, BF16),
        vm((rows, width), BF16),
        vm((width, ff), BF16),
        vm((width, ff), BF16),
        vm((ff, width), BF16),
        vm((width, 2 * unit), BF16),
        vm((unit, width), BF16),
        vm((span, query_rows.shape[1]), BF16),
        vm((span, width), BF16),
        vm((nx, rows, width), BF16),
        vm((rows, width), F32),
        vm((nx * rows, width), BF16),
        vm((nx * rows, width), BF16),
        vm((nx, rows, width), BF16),
        vm((NCH, nz * rows, cw), BF16),
        vm((nz, 16, 128), F32),
        vm((groups, plane * group_rows, 256), BF16),
        vm((groups, 256, plane * group_rows), BF16),
        vm((groups, plane * group_rows, width), BF16),
        vm((groups, plane * group_rows, width), BF16),
        vm((groups, plane * group_rows, width), BF16),
        vm((groups, plane * group_rows, width), BF16),
        vm(((nz - 1) * rows, width), F32),
        vm((rows, width), F32),
        vm((2, half, NCH, rows, cw), BF16),
        vm((2, half, NCH, rows, cw), BF16),
        dma((11,)),
        dma((2,)),
        dma((2,)),
        dma((nx,)),
        dma((nx,)),
        dma((nx,)),
        dma((nx,)),
        dma((nx,)),
        dma((nx,)),
        dma((2, half, NCH)),
        dma((nz, NCH)),
        dma((2, half)),
        dma((nz,)),
        dma((groups, plane)),
        dma((groups, plane)),
        dma((groups, plane)),
        dma((groups, plane)),
        dma((2, half, NCH)),
        dma((2, half, NCH)),
    ]
    hbm = pl.BlockSpec(memory_space=pl.ANY)
    vmem = pl.BlockSpec(memory_space=pltpu.VMEM)
    smem = pl.BlockSpec(memory_space=pltpu.SMEM)
    return pl.pallas_call(
        functools.partial(kernel, nz, nx),
        out_shape=jax.ShapeDtypeStruct((rows, width), BF16),
        in_specs=[
            hbm,
            hbm,
            hbm,
            smem,
            hbm,
            hbm,
            vmem,
            vmem,
            vmem,
            hbm,
            hbm,
            hbm,
            hbm,
            hbm,
            hbm,
        ],
        out_specs=vmem,
        scratch_shapes=scratch,
        compiler_params=pltpu.CompilerParams(
            collective_id=0, has_side_effects=True, vmem_limit_bytes=60 * 1024 * 1024
        ),
    )(
        query_rows,
        key_rows,
        value_rows,
        sink_logit,
        out_weight,
        residual,
        norm_gain.reshape(1, width),
        routes,
        gate_weights,
        expert_gate,
        expert_up,
        expert_down,
        shared_gate,
        shared_up,
        shared_down,
    )


def solution(mesh):
    placed = (
        P(("grp", "sp"), "tp"),
        P(("grp", "sp"), "tp"),
        P(("grp", "sp"), "tp"),
        P("tp"),
        P("tp", None),
        P(("grp", "sp", "tp"), None),
        P(),
        P(("grp", "sp", "tp"), None),
        P(("grp", "sp", "tp"), None),
        P(("sp", "tp"), None, None),
        P(("sp", "tp"), None, None),
        P(("sp", "tp"), None, None),
        P(None, "tp"),
        P(None, "tp"),
        P("tp", None),
    )
    return jax.shard_map(
        functools.partial(body, mesh.shape["sp"] // 2, mesh.shape["tp"]),
        mesh=mesh,
        in_specs=placed,
        out_specs=P(("grp", "sp", "tp"), None),
        check_vma=False,
    )
```

```python
import functools

import jax
import jax.numpy as jnp
from jax import lax
from jax.experimental import pallas as pl
from jax.experimental.pallas import tpu as pltpu
from jax.sharding import PartitionSpec as P

HEAD = 64
WINDOW = 128
TOPK = 6
CAP = 3
NCH = 4
PER = 5
LAG = 0.45
NORM_EPS = 1e-06
MESH = pl.DeviceIdType.MESH
F32 = jnp.float32
BF16 = jnp.bfloat16


def iota(shape, dim):
    return lax.broadcasted_iota(jnp.int32, shape, dim)


def dot(a, b):
    return jnp.dot(a, b, preferred_element_type=F32)


def silu(v):
    return v / (1.0 + jnp.exp(-v))


def kernel(
    nz,
    nx,
    q_hbm,
    k_hbm,
    v_hbm,
    sink_hbm,
    ow_hbm,
    res_hbm,
    gain_hbm,
    routes_hbm,
    gw_hbm,
    eg_hbm,
    eu_hbm,
    ed_hbm,
    sg_hbm,
    su_hbm,
    sd_hbm,
    out_ref,
    sinks,
    gain,
    ids,
    gates,
    qb,
    kv,
    ow,
    res,
    eg,
    eu,
    ed,
    wsh,
    sd,
    att,
    pbuf,
    precv,
    stream,
    slab,
    shp,
    shr,
    ag,
    meta,
    sel,
    com,
    sb,
    rb,
    eo,
    cb,
    acc,
    part,
    own,
    rsr,
    rss,
    lsem,
    hsend,
    hrecv,
    psend,
    pecv,
    nsend,
    nrecv,
    ssend,
    srecv,
    agsend,
    agrecv,
    msend,
    mrecv,
    dsend,
    drecv,
    csend,
    crecv,
    dsend2,
    drecv2,
    csend2,
    crecv2,
    rsend,
    rrecv,
):
    rows, width = res.shape
    cw = width // NCH
    half = nz // 2
    plane = 2 * nx
    groups = (nz - 1) // PER
    group_rows = PER * CAP + 1
    order = [0]
    for k in range(1, half):
        order += [k, -k]
    order.append(half)
    slot = {d: i for i, d in enumerate(order)}
    slot[-half] = slot[half]

    sp = lax.axis_index("sp")
    x = lax.axis_index("tp")
    nsp = 2 * nz
    z = sp // 2
    c = sp % 2
    zs = ((z + 1) % nz, (z + nz - 1) % nz)

    def at(z_, c_, x_):
        return {"sp": z_ * 2 + c_, "tp": x_}

    def mate(q):
        dc, dx = q // nx, q % nx
        return (c if dc == 0 else 1 - c), (x + dx) % nx

    def back(q):
        dc, dx = q // nx, q % nx
        return dc * nx + (nx - dx) % nx

    sent = []

    def send(src, dst, ss, rs, device):
        copy = pltpu.make_async_remote_copy(
            src_ref=src,
            dst_ref=dst,
            send_sem=ss,
            recv_sem=rs,
            device_id=device,
            device_id_type=MESH,
        )
        copy.start()
        sent.append(copy)

    me = at(z, c, x)

    def arrived(dst, rs):
        pltpu.make_async_remote_copy(
            src_ref=dst,
            dst_ref=dst,
            send_sem=rs,
            recv_sem=rs,
            device_id=me,
            device_id_type=MESH,
        ).wait_recv()

    barrier = pltpu.get_barrier_semaphore()
    cross = at((z + nz + 2 * c - 1) % nz, 1 - c, x)
    friends = [cross, at(zs[0], c, x), at(zs[1], c, x)]
    for q in range(1, plane):
        cq, xq = mate(q)
        friends.append(at(z, cq, xq))
    for friend in friends:
        pl.semaphore_signal(barrier, inc=1, device_id=friend, device_id_type=MESH)

    loads = []

    def load(src, dst):
        copy = pltpu.make_async_copy(src, dst, lsem.at[len(loads)])
        copy.start()
        loads.append(copy)
        return copy

    span = kv.shape[1] // 3
    load_k = load(k_hbm, kv.at[0, span : 2 * span])
    load_v = load(v_hbm, kv.at[1, span : 2 * span])
    load_q = load(q_hbm, qb)
    load_ids = load(routes_hbm, ids)
    load_gates = load(gw_hbm, gates)
    load_sink = load(sink_hbm, sinks)
    load_ow = load(ow_hbm, ow)
    load_res = load(res_hbm, res)
    load_gain = load(gain_hbm, gain)
    unit = sg_hbm.shape[1]
    load_eg = load(eg_hbm.at[0], eg)
    load_eu = load(eu_hbm.at[0], eu)
    load_ed = load(ed_hbm.at[0], ed)
    load_sg = load(sg_hbm, wsh.at[:, 0:unit])
    load_su = load(su_hbm, wsh.at[:, unit : 2 * unit])
    load_sd = load(sd_hbm, sd)

    load_k.wait()
    load_v.wait()
    pl.semaphore_wait(barrier, len(friends))

    mine = kv.at[:, span : 2 * span, :]
    nxt = {"sp": (sp + 1) % nsp, "tp": x}
    prv = {"sp": (sp + nsp - 1) % nsp, "tp": x}
    send(mine, kv.at[:, 0:span, :], hsend.at[0], hrecv.at[0], nxt)
    send(mine, kv.at[:, 2 * span : 3 * span, :], hsend.at[1], hrecv.at[1], prv)

    load_ids.wait()
    load_gates.wait()
    lane = iota((rows, 128), 1)
    spread = jnp.where((lane & (rows - 1)) == iota((rows, 128), 0), 1.0, 0.0).astype(BF16)
    named = dot(ids[...].astype(F32).astype(BF16), spread)
    rest = gates[...]
    weighted = jnp.zeros((TOPK, 128), F32)
    for _ in range(3):
        high = rest.astype(BF16)
        weighted = weighted + dot(high, spread)
        rest = rest - high.astype(F32)
    names = iota((128, 128), 0).astype(F32)
    hot = jnp.zeros((128, 128), F32)
    for k in range(TOPK):
        hot = hot + jnp.where(names == named[k : k + 1, :], 1.0, 0.0)
    sub, on = iota((128, 128), 0), iota((128, 128), 1)
    earlier = jnp.where((sub < (on & (rows - 1))) & (sub < rows), 1.0, 0.0)
    before = dot(hot.astype(BF16), earlier.astype(BF16))
    meta[0] = jnp.full((16, 128), -4.0, F32)
    for k in range(TOPK):
        rank = jnp.sum(
            jnp.where(names == named[k : k + 1, :], before, 0.0), axis=0, keepdims=True
        )
        meta[0, k : k + 1, :] = 4.0 * named[k : k + 1, :] + rank
        meta[0, 8 + k : 9 + k, :] = weighted[k : k + 1, :]

    load_q.wait()
    lane_q = iota((span, 128), 1)
    low = lane_q < HEAD
    heads = []
    for h in range(2 * (qb.shape[1] // 128)):
        pair = qb[:, (h // 2) * 128 : (h // 2) * 128 + 128].astype(F32)
        if h % 2 != h // 2:
            pair = pltpu.roll(pair, HEAD, 1)
        keep = low if h // 2 == 0 else jnp.logical_not(low)
        heads.append(jnp.where(keep, pair, 0.0).astype(BF16))

    row_i = iota((span, 3 * span), 0)
    col_i = iota((span, 3 * span), 1)
    pos = sp * span - span + col_i
    open_ = (col_i >= row_i) & (col_i <= row_i + 2 * WINDOW) & (pos >= 0) & (pos < nsp * span)
    arrived(kv.at[:, 0:span, :], hrecv.at[0])
    arrived(kv.at[:, 2 * span : 3 * span, :], hrecv.at[1])
    load_sink.wait()
    keys = kv[0]
    values = kv[1]
    results = []
    for h, query in enumerate(heads):
        scores = lax.dot_general(
            query, keys, (((1,), (1,)), ((), ())), preferred_element_type=F32
        ) * (HEAD**-0.5)
        scores = jnp.where(open_, scores, -jnp.inf)
        sink = sinks[h]
        row_max = jnp.maximum(jnp.max(scores, axis=-1, keepdims=True), sink)
        shifted = jnp.exp(scores - row_max)
        denominator = jnp.exp(sink - row_max) + jnp.sum(shifted, axis=-1, keepdims=True)
        weights = (shifted / denominator).astype(BF16)
        got = dot(weights, values)
        if h % 2 != h // 2:
            got = pltpu.roll(got, HEAD, 1)
        results.append(got)
    for pair in range(len(heads) // 2):
        att[:, pair * 128 : pair * 128 + 128] = jnp.where(
            low, results[2 * pair], results[2 * pair + 1]
        ).astype(BF16)

    load_ow.wait()
    attended = att[...]
    for ch in range(NCH):
        cols = slice(ch * cw, (ch + 1) * cw)
        pbuf[:, cols] = dot(attended, ow[:, cols]).astype(BF16)
    for dx in (2, 1, 3):
        xq = (x + dx) % nx
        there = (nx - dx) % nx
        begin = pl.multiple_of(xq * rows, rows)
        send(
            pbuf.at[pl.ds(begin, rows), :],
            precv.at[there],
            psend.at[dx],
            pecv.at[there],
            at(z, c, xq),
        )
    load_res.wait()
    load_gain.wait()
    total = res[...].astype(F32) + pbuf[pl.ds(pl.multiple_of(x * rows, rows), rows), :].astype(F32)
    for dx in range(1, nx):
        arrived(precv.at[dx], pecv.at[dx])
    for dx in range(1, nx):
        total = total + precv[dx].astype(F32)
    stream[...] = total
    scale = lax.rsqrt(jnp.mean(total * total, axis=-1, keepdims=True) + NORM_EPS)
    normed = (total * scale * gain[...]).astype(BF16)
    slab[0:rows, :] = normed
    for ch in range(NCH):
        ag[ch, 0:rows, :] = normed[:, ch * cw : (ch + 1) * cw]

    def carries(direction, step, ch):
        return step < half or (step == half and (ch < NCH // 2) == (direction == 0))

    def source(direction, step):
        return slot[-step if direction == 0 else step]

    def block(ch, s):
        return ag.at[ch, s * rows : (s + 1) * rows, :]

    def forward(step, ch, direction):
        if not carries(direction, step, ch):
            return
        a, b = source(direction, step - 1), source(direction, step)
        send(
            block(ch, a),
            block(ch, b),
            agsend.at[direction, step - 1, ch],
            agrecv.at[b, ch],
            at(zs[direction], c, x),
        )

    def forward_meta(step, direction):
        if step == half and direction == 1:
            return
        a, b = source(direction, step - 1), source(direction, step)
        send(
            meta.at[a],
            meta.at[b],
            msend.at[direction, step - 1],
            mrecv.at[b],
            at(zs[direction], c, x),
        )

    def gather_meta(step):
        for direction in range(2):
            if not (step == half and direction == 1):
                t = source(direction, step)
                arrived(meta.at[t], mrecv.at[t])
                if step < half:
                    forward_meta(step + 1, direction)

    def gather_chunk(step, ch):
        for direction in range(2):
            if carries(direction, step, ch):
                t = source(direction, step)
                arrived(block(ch, t), agrecv.at[t, ch])
                if step < half:
                    forward(step + 1, ch, direction)

    def gather_step(step):
        gather_meta(step)
        for ch in range(NCH):
            gather_chunk(step, ch)

    for direction in range(2):
        forward_meta(1, direction)
    for ch in range(NCH):
        for direction in range(2):
            forward(1, ch, direction)
    for dx in (2, 1, 3):
        there = (nx - dx) % nx
        send(
            slab.at[0:rows, :],
            slab.at[there * rows : (there + 1) * rows, :],
            nsend.at[dx],
            nrecv.at[there],
            at(z, c, (x + dx) % nx),
        )

    def shared_expert():
        for dx in range(1, nx):
            arrived(slab.at[dx * rows : (dx + 1) * rows, :], nrecv.at[dx])
        load_sg.wait()
        load_su.wait()
        load_sd.wait()
        both = dot(slab[...], wsh[...])
        hidden = (silu(both[:, 0:unit]) * both[:, unit : 2 * unit]).astype(BF16)
        for ch in range(NCH):
            cols = slice(ch * cw, (ch + 1) * cw)
            shp[:, cols] = dot(hidden, sd[:, cols]).astype(BF16)

    def shared_out():
        for dx in (2, 1, 3):
            there = (nx - dx) % nx
            send(
                shp.at[dx * rows : (dx + 1) * rows, :],
                shr.at[there],
                ssend.at[dx],
                srecv.at[there],
                at(z, c, (x + dx) % nx),
            )

    def build(g):
        lane8 = iota((8, 128), 1)
        seg8 = lane8 // rows
        codes, gws = [], []
        for v in range(2):
            code = jnp.full((8, 128), -4.0, F32)
            gate = jnp.zeros((8, 128), F32)
            for i in range(4):
                p = 4 * v + i
                if p > PER:
                    continue
                s = 0 if p == 0 else PER * g + p
                code = jnp.where(seg8 == i, meta[s, 0:8, :], code)
                gate = jnp.where(seg8 == i, meta[s, 8:16, :], gate)
            codes.append(code)
            gws.append(gate)
        rr = iota((group_rows, 128), 0)
        bi = (rr * 11) >> 5
        last = rr == group_rows - 1
        pos_r = jnp.where(last, 0, 1 + bi)
        rank_r = jnp.where(last, g, rr - 3 * bi)
        seg = iota((group_rows, 128), 1) // rows
        turned = []
        for q in range(plane):
            cq, xq = mate(q)
            expert = plane * z + nx * cq + xq
            want = (rank_r + 4 * expert).astype(F32)
            lines = []
            for v in range(2):
                placed = pos_r == seg + 4 * v
                one = jnp.zeros((group_rows, 128), F32)
                weight = jnp.zeros((group_rows, 128), F32)
                for k in range(TOPK):
                    match = (codes[v][k : k + 1, :] == want) & placed
                    one = jnp.where(match, 1.0, one)
                    weight = jnp.where(match, gws[v][k : k + 1, :], weight)
                sel[g, q * group_rows : (q + 1) * group_rows, v * 128 : (v + 1) * 128] = one.astype(
                    BF16
                )
                lines.append(weight)
            turned.append(lines)
        for v in range(2):
            column = jnp.concatenate([turned[q][v] for q in range(plane)], axis=0)
            com[g, v * 128 : (v + 1) * 128, :] = column.T.astype(BF16)

    far = [2, nx + 2, 1, nx + 1, 3, nx + 3, nx]
    final = groups - 1

    def part_of(q):
        return slice(q * group_rows, (q + 1) * group_rows)

    def columns(ch):
        return slice(ch * cw, (ch + 1) * cw)

    def swap(g, ch, src, dst, ss, rs, ss2, rs2):
        for q in far:
            cq, xq = mate(q)
            b = back(q)
            if ch is None:
                send(
                    src.at[g, :, part_of(q), :],
                    dst.at[g, :, part_of(b), :],
                    ss.at[g, q],
                    rs.at[g, b],
                    at(z, cq, xq),
                )
            else:
                send(
                    src.at[g, ch, part_of(q), :],
                    dst.at[g, ch, part_of(b), :],
                    ss2.at[ch, q],
                    rs2.at[ch, b],
                    at(z, cq, xq),
                )

    def came(g, ch, dst, rs, rs2):
        for q in range(1, plane):
            if g < final:
                arrived(dst.at[g, :, part_of(q), :], rs.at[g, q])
            else:
                arrived(dst.at[g, ch, part_of(q), :], rs2.at[ch, q])

    def pick(g, ch):
        first = ag[ch, 0:rows, :]
        begin = (1 + PER * g) * rows
        stack = jnp.concatenate(
            [first, ag[ch, begin : begin + PER * rows, :], first, first], axis=0
        )
        picked = dot(sel[g], stack).astype(BF16)
        rb[g, ch, 0:group_rows, :] = picked[0:group_rows]
        sb[g, ch, group_rows:, :] = picked[group_rows:]

    def dispatch(g):
        build(g)
        for ch in range(NCH):
            pick(g, ch)
        swap(g, None, sb, rb, dsend, drecv, dsend2, drecv2)

    def enter(g, ch):
        rows_in = rb[g, ch]
        gate = dot(rows_in, eg[columns(ch), :])
        up = dot(rows_in, eu[columns(ch), :])
        if ch == 0:
            acc[0] = gate
            acc[1] = up
        else:
            acc[0] = acc[0] + gate
            acc[1] = acc[1] + up

    def leave(g, ch, hidden):
        made = dot(hidden, ed[:, columns(ch)]).astype(BF16)
        cb[g, ch, 0:group_rows, :] = made[0:group_rows]
        eo[g, ch, group_rows:, :] = made[group_rows:]

    def experts(g):
        came(g, None, rb, drecv, drecv2)
        taken = [rb[g, ch] for ch in range(NCH)]
        taken = jnp.concatenate(taken, axis=1)
        hidden = (silu(dot(taken, eg[...])) * dot(taken, eu[...])).astype(BF16)
        for ch in range(NCH):
            leave(g, ch, hidden)

    def give_back(g, ch):
        swap(g, ch, eo, cb, csend, crecv, csend2, crecv2)

    def combine(g, ch):
        used = (PER + 1) * rows
        summed = dot(com[g, 0:used, :], cb[g, ch])
        cols = columns(ch)
        if g == 0:
            own[:, cols] = summed[0:rows]
        else:
            own[:, cols] = own[:, cols] + summed[0:rows]
        part[g * PER * rows : (g + 1) * PER * rows, cols] = summed[rows:used]

    def combine_all(g):
        came(g, None, cb, crecv, crecv2)
        for ch in range(NCH):
            combine(g, ch)

    gather_step(1)
    gather_step(2)
    gather_step(3)
    dispatch(0)
    gather_step(4)
    gather_step(5)
    dispatch(1)
    gather_step(6)
    load_eg.wait()
    load_eu.wait()
    load_ed.wait()
    experts(0)
    give_back(0, None)
    gather_step(7)
    gather_meta(8)
    build(final)
    for ch in range(NCH):
        gather_chunk(8, ch)
        pick(final, ch)
        swap(final, ch, sb, rb, dsend, drecv, dsend2, drecv2)
    experts(1)
    shared_expert()
    combine_all(0)
    for ch in range(NCH):
        came(final, ch, rb, drecv, drecv2)
        enter(final, ch)
    hidden = (silu(acc[0]) * acc[1]).astype(BF16)
    for ch in range(NCH):
        leave(final, ch, hidden)
        give_back(final, ch)
    give_back(1, None)
    shared_out()

    def brings(direction, step, ch):
        return step > 1 or (ch < NCH // 2) == (direction == 0)

    def reduce_chunk(step, ch):
        distance = half + 1 - step
        for direction in range(2):
            if not brings(direction, step, ch):
                continue
            s = slot[distance if direction == 0 else -distance]
            value = part[(s - 1) * rows : s * rows, columns(ch)]
            if step > 1 and brings(direction, step - 1, ch):
                arrived(rsr.at[direction, step - 2, ch], rrecv.at[direction, step - 2, ch])
                value = value + rsr[direction, step - 2, ch].astype(F32)
            rss[direction, step - 1, ch] = value.astype(BF16)
            send(
                rss.at[direction, step - 1, ch],
                rsr.at[direction, step - 1, ch],
                rsend.at[direction, step - 1, ch],
                rrecv.at[direction, step - 1, ch],
                at(zs[direction], c, x),
            )

    events = sorted(
        (step + LAG * ch, step, ch) for step in range(1, half + 1) for ch in range(NCH)
    )
    merged = False
    for _, step, ch in events:
        if step == 1:
            came(final, ch, cb, crecv, crecv2)
            combine(final, ch)
        if step == 4 and not merged:
            combine_all(1)
            merged = True
        reduce_chunk(step, ch)

    base = stream[...] + shp[0:rows, :].astype(F32)
    for dx in range(1, nx):
        arrived(shr.at[dx], srecv.at[dx])
        base = base + shr[dx].astype(F32)
    stream[...] = base + own[...]
    for ch in range(NCH):
        cols = slice(ch * cw, (ch + 1) * cw)
        value = stream[:, cols]
        for direction in range(2):
            arrived(rsr.at[direction, half - 1, ch], rrecv.at[direction, half - 1, ch])
            value = value + rsr[direction, half - 1, ch].astype(F32)
        out_ref[:, cols] = value.astype(BF16)
    for copy in sent:
        copy.wait_send()


def body(nz, nx, *args):
    (
        query_rows,
        key_rows,
        value_rows,
        sink_logit,
        out_weight,
        residual,
        norm_gain,
        routes,
        gate_weights,
        expert_gate,
        expert_up,
        expert_down,
        shared_gate,
        shared_up,
        shared_down,
    ) = args
    rows, width = residual.shape
    span = query_rows.shape[0]
    half = nz // 2
    plane = 2 * nx
    groups = (nz - 1) // PER
    group_rows = PER * CAP + 1
    cw = width // NCH
    ff = expert_gate.shape[2]
    unit = shared_gate.shape[1]
    dma = pltpu.SemaphoreType.DMA
    vm = pltpu.VMEM
    scratch = [
        pltpu.SMEM(sink_logit.shape, F32),
        vm((1, width), F32),
        vm((TOPK, rows), jnp.int32),
        vm((TOPK, rows), F32),
        vm((span, query_rows.shape[1]), BF16),
        vm((2, 3 * span, key_rows.shape[1]), BF16),
        vm(out_weight.shape, BF16),
        vm((rows, width), BF16),
        vm((width, ff), BF16),
        vm((width, ff), BF16),
        vm((ff, width), BF16),
        vm((width, 2 * unit), BF16),
        vm((unit, width), BF16),
        vm((span, query_rows.shape[1]), BF16),
        vm((span, width), BF16),
        vm((nx, rows, width), BF16),
        vm((rows, width), F32),
        vm((nx * rows, width), BF16),
        vm((nx * rows, width), BF16),
        vm((nx, rows, width), BF16),
        vm((NCH, nz * rows, cw), BF16),
        vm((nz, 16, 128), F32),
        vm((groups, plane * group_rows, 256), BF16),
        vm((groups, 256, plane * group_rows), BF16),
        vm((groups, NCH, plane * group_rows, cw), BF16),
        vm((groups, NCH, plane * group_rows, cw), BF16),
        vm((groups, NCH, plane * group_rows, cw), BF16),
        vm((groups, NCH, plane * group_rows, cw), BF16),
        vm((2, plane * group_rows, ff), F32),
        vm(((nz - 1) * rows, width), F32),
        vm((rows, width), F32),
        vm((2, half, NCH, rows, cw), BF16),
        vm((2, half, NCH, rows, cw), BF16),
        dma((15,)),
        dma((2,)),
        dma((2,)),
        dma((nx,)),
        dma((nx,)),
        dma((nx,)),
        dma((nx,)),
        dma((nx,)),
        dma((nx,)),
        dma((2, half, NCH)),
        dma((nz, NCH)),
        dma((2, half)),
        dma((nz,)),
        dma((groups - 1, plane)),
        dma((groups - 1, plane)),
        dma((groups - 1, plane)),
        dma((groups - 1, plane)),
        dma((NCH, plane)),
        dma((NCH, plane)),
        dma((NCH, plane)),
        dma((NCH, plane)),
        dma((2, half, NCH)),
        dma((2, half, NCH)),
    ]
    hbm = pl.BlockSpec(memory_space=pl.ANY)
    vmem = pl.BlockSpec(memory_space=pltpu.VMEM)
    return pl.pallas_call(
        functools.partial(kernel, nz, nx),
        out_shape=jax.ShapeDtypeStruct((rows, width), BF16),
        in_specs=[hbm] * 15,
        out_specs=vmem,
        scratch_shapes=scratch,
        compiler_params=pltpu.CompilerParams(
            collective_id=0, has_side_effects=True, vmem_limit_bytes=60 * 1024 * 1024
        ),
    )(
        query_rows,
        key_rows,
        value_rows,
        sink_logit,
        out_weight,
        residual,
        norm_gain.reshape(1, width),
        routes.T,
        gate_weights.T,
        expert_gate,
        expert_up,
        expert_down,
        shared_gate,
        shared_up,
        shared_down,
    )


def solution(mesh):
    placed = (
        P(("grp", "sp"), "tp"),
        P(("grp", "sp"), "tp"),
        P(("grp", "sp"), "tp"),
        P("tp"),
        P("tp", None),
        P(("grp", "sp", "tp"), None),
        P(),
        P(("grp", "sp", "tp"), None),
        P(("grp", "sp", "tp"), None),
        P(("sp", "tp"), None, None),
        P(("sp", "tp"), None, None),
        P(("sp", "tp"), None, None),
        P(None, "tp"),
        P(None, "tp"),
        P("tp", None),
    )
    return jax.shard_map(
        functools.partial(body, mesh.shape["sp"] // 2, mesh.shape["tp"]),
        mesh=mesh,
        in_specs=placed,
        out_specs=P(("grp", "sp", "tp"), None),
        check_vma=False,
    )
```

```python
import functools

import jax
import jax.numpy as jnp
from jax import lax
from jax.experimental import pallas as pl
from jax.experimental.pallas import tpu as pltpu
from jax.sharding import PartitionSpec as P

HEAD = 64
WINDOW = 128
TOPK = 6
CAP = 3
NCH = 4
PER = 5
LAG = 0.45
NORM_EPS = 1e-06
MESH = pl.DeviceIdType.MESH
F32 = jnp.float32
BF16 = jnp.bfloat16


def iota(shape, dim):
    return lax.broadcasted_iota(jnp.int32, shape, dim)


def dot(a, b):
    return jnp.dot(a, b, preferred_element_type=F32)


def silu(v):
    return v / (1.0 + jnp.exp(-v))


def kernel(
    nz,
    nx,
    q_hbm,
    k_hbm,
    v_hbm,
    sink_hbm,
    ow_hbm,
    res_hbm,
    gain_hbm,
    routes_hbm,
    gw_hbm,
    eg_hbm,
    eu_hbm,
    ed_hbm,
    sg_hbm,
    su_hbm,
    sd_hbm,
    out_ref,
    sinks,
    gain,
    ids,
    gates,
    qb,
    kv,
    ow,
    res,
    eg,
    eu,
    ed,
    wsh,
    sd,
    att,
    pbuf,
    precv,
    stream,
    slab,
    shp,
    shr,
    ag,
    meta,
    sel,
    com,
    sb,
    rb,
    eo,
    cb,
    acc,
    part,
    own,
    staged,
    rsr,
    rss,
    lsem,
    hsend,
    hrecv,
    psend,
    pecv,
    nsend,
    nrecv,
    ssend,
    srecv,
    agsend,
    agrecv,
    msend,
    mrecv,
    dsend,
    drecv,
    csend,
    crecv,
    dsend2,
    drecv2,
    csend2,
    crecv2,
    rsend,
    rrecv,
):
    rows, width = res.shape
    cw = width // NCH
    half = nz // 2
    plane = 2 * nx
    groups = (nz - 1) // PER
    group_rows = PER * CAP + 1
    order = [0]
    for k in range(1, half):
        order += [k, -k]
    order.append(half)
    slot = {d: i for i, d in enumerate(order)}
    slot[-half] = slot[half]

    sp = lax.axis_index("sp")
    x = lax.axis_index("tp")
    nsp = 2 * nz
    z = sp // 2
    c = sp % 2
    zs = ((z + 1) % nz, (z + nz - 1) % nz)

    def at(z_, c_, x_):
        return {"sp": z_ * 2 + c_, "tp": x_}

    def mate(q):
        dc, dx = q // nx, q % nx
        return (c if dc == 0 else 1 - c), (x + dx) % nx

    def back(q):
        dc, dx = q // nx, q % nx
        return dc * nx + (nx - dx) % nx

    sent = []

    def send(src, dst, ss, rs, device):
        copy = pltpu.make_async_remote_copy(
            src_ref=src,
            dst_ref=dst,
            send_sem=ss,
            recv_sem=rs,
            device_id=device,
            device_id_type=MESH,
        )
        copy.start()
        sent.append(copy)

    me = at(z, c, x)

    def arrived(dst, rs):
        pltpu.make_async_remote_copy(
            src_ref=dst,
            dst_ref=dst,
            send_sem=rs,
            recv_sem=rs,
            device_id=me,
            device_id_type=MESH,
        ).wait_recv()

    barrier = pltpu.get_barrier_semaphore()
    cross = at((z + nz + 2 * c - 1) % nz, 1 - c, x)
    friends = [cross, at(zs[0], c, x), at(zs[1], c, x)]
    for q in range(1, plane):
        cq, xq = mate(q)
        friends.append(at(z, cq, xq))
    for friend in friends:
        pl.semaphore_signal(barrier, inc=1, device_id=friend, device_id_type=MESH)

    loads = []

    def load(src, dst):
        copy = pltpu.make_async_copy(src, dst, lsem.at[len(loads)])
        copy.start()
        loads.append(copy)
        return copy

    span = kv.shape[1] // 3
    load_k = load(k_hbm, kv.at[0, span : 2 * span])
    load_v = load(v_hbm, kv.at[1, span : 2 * span])
    load_q = load(q_hbm, qb)
    load_ids = load(routes_hbm, ids)
    load_gates = load(gw_hbm, gates)
    load_sink = load(sink_hbm, sinks)
    load_ow = load(ow_hbm, ow)
    load_res = load(res_hbm, res)
    load_gain = load(gain_hbm, gain)
    unit = sg_hbm.shape[1]
    load_eg = load(eg_hbm.at[0], eg)
    load_eu = load(eu_hbm.at[0], eu)
    load_ed = load(ed_hbm.at[0], ed)
    load_sg = load(sg_hbm, wsh.at[:, 0:unit])
    load_su = load(su_hbm, wsh.at[:, unit : 2 * unit])
    load_sd = load(sd_hbm, sd)

    load_k.wait()
    load_v.wait()
    pl.semaphore_wait(barrier, len(friends))

    mine = kv.at[:, span : 2 * span, :]
    nxt = {"sp": (sp + 1) % nsp, "tp": x}
    prv = {"sp": (sp + nsp - 1) % nsp, "tp": x}
    send(mine, kv.at[:, 0:span, :], hsend.at[0], hrecv.at[0], nxt)
    send(mine, kv.at[:, 2 * span : 3 * span, :], hsend.at[1], hrecv.at[1], prv)

    load_ids.wait()
    load_gates.wait()
    lane = iota((rows, 128), 1)
    line = iota((rows, 128), 0)
    first_seg = jnp.where(lane == line, 1.0, 0.0).astype(BF16)
    second_seg = jnp.where(lane == line + rows, 1.0, 0.0).astype(BF16)
    named = dot(ids[...].astype(F32).astype(BF16), first_seg)
    rest = gates[...]
    weighted = jnp.zeros((TOPK, 128), F32)
    for _ in range(3):
        high = rest.astype(BF16)
        weighted = weighted + dot(high, second_seg)
        rest = rest - high.astype(F32)
    names = iota((128, 128), 0).astype(F32)
    hot = jnp.zeros((128, 128), F32)
    for k in range(TOPK):
        hot = hot + jnp.where(names == named[k : k + 1, :], 1.0, 0.0)
    sub, on = iota((128, 128), 0), iota((128, 128), 1)
    earlier = jnp.where((sub < (on & (rows - 1))) & (sub < rows), 1.0, 0.0)
    before = dot(hot.astype(BF16), earlier.astype(BF16))
    segment = iota((1, 128), 1) // rows
    meta[0] = jnp.full((8, 128), -4.0, F32)
    for k in range(TOPK):
        name = named[k : k + 1, :]
        rank = jnp.sum(jnp.where(names == name, before, 0.0), axis=0, keepdims=True)
        meta[0, k : k + 1, :] = jnp.where(
            segment == 0, 4.0 * name + rank, weighted[k : k + 1, :]
        )

    load_q.wait()
    lane_q = iota((span, 128), 1)
    low = lane_q < HEAD
    heads = []
    for h in range(2 * (qb.shape[1] // 128)):
        pair = qb[:, (h // 2) * 128 : (h // 2) * 128 + 128].astype(F32)
        if h % 2 != h // 2:
            pair = pltpu.roll(pair, HEAD, 1)
        keep = low if h // 2 == 0 else jnp.logical_not(low)
        heads.append(jnp.where(keep, pair, 0.0).astype(BF16))

    row_i = iota((span, 3 * span), 0)
    col_i = iota((span, 3 * span), 1)
    pos = sp * span - span + col_i
    open_ = (col_i >= row_i) & (col_i <= row_i + 2 * WINDOW) & (pos >= 0) & (pos < nsp * span)
    arrived(kv.at[:, 0:span, :], hrecv.at[0])
    arrived(kv.at[:, 2 * span : 3 * span, :], hrecv.at[1])
    load_sink.wait()
    keys = kv[0]
    values = kv[1]
    results = []
    for h, query in enumerate(heads):
        scores = lax.dot_general(
            query, keys, (((1,), (1,)), ((), ())), preferred_element_type=F32
        ) * (HEAD**-0.5)
        scores = jnp.where(open_, scores, -jnp.inf)
        sink = sinks[h]
        row_max = jnp.maximum(jnp.max(scores, axis=-1, keepdims=True), sink)
        shifted = jnp.exp(scores - row_max)
        denominator = jnp.exp(sink - row_max) + jnp.sum(shifted, axis=-1, keepdims=True)
        weights = (shifted / denominator).astype(BF16)
        got = dot(weights, values)
        if h % 2 != h // 2:
            got = pltpu.roll(got, HEAD, 1)
        results.append(got)
    for pair in range(len(heads) // 2):
        att[:, pair * 128 : pair * 128 + 128] = jnp.where(
            low, results[2 * pair], results[2 * pair + 1]
        ).astype(BF16)

    load_ow.wait()
    attended = att[...]
    for ch in range(NCH):
        cols = slice(ch * cw, (ch + 1) * cw)
        pbuf[:, cols] = dot(attended, ow[:, cols]).astype(BF16)
    for dx in (2, 1, 3):
        xq = (x + dx) % nx
        there = (nx - dx) % nx
        begin = pl.multiple_of(xq * rows, rows)
        send(
            pbuf.at[pl.ds(begin, rows), :],
            precv.at[there],
            psend.at[dx],
            pecv.at[there],
            at(z, c, xq),
        )
    load_res.wait()
    load_gain.wait()
    total = res[...].astype(F32) + pbuf[pl.ds(pl.multiple_of(x * rows, rows), rows), :].astype(F32)
    for dx in range(1, nx):
        arrived(precv.at[dx], pecv.at[dx])
    for dx in range(1, nx):
        total = total + precv[dx].astype(F32)
    stream[...] = total
    scale = lax.rsqrt(jnp.mean(total * total, axis=-1, keepdims=True) + NORM_EPS)
    normed = (total * scale * gain[...]).astype(BF16)
    slab[0:rows, :] = normed
    for ch in range(NCH):
        ag[ch, 0:rows, :] = normed[:, ch * cw : (ch + 1) * cw]

    def carries(direction, step, ch):
        return step < half or (step == half and (ch < NCH // 2) == (direction == 0))

    def source(direction, step):
        return slot[-step if direction == 0 else step]

    def block(ch, s):
        return ag.at[ch, s * rows : (s + 1) * rows, :]

    def forward(step, ch, direction):
        if not carries(direction, step, ch):
            return
        a, b = source(direction, step - 1), source(direction, step)
        send(
            block(ch, a),
            block(ch, b),
            agsend.at[direction, step - 1, ch],
            agrecv.at[b, ch],
            at(zs[direction], c, x),
        )

    def forward_meta(step, direction):
        if step == half and direction == 1:
            return
        a, b = source(direction, step - 1), source(direction, step)
        send(
            meta.at[a],
            meta.at[b],
            msend.at[direction, step - 1],
            mrecv.at[b],
            at(zs[direction], c, x),
        )

    def gather_meta(step):
        for direction in range(2):
            if not (step == half and direction == 1):
                t = source(direction, step)
                arrived(meta.at[t], mrecv.at[t])
                if step < half:
                    forward_meta(step + 1, direction)

    def gather_chunk(step, ch):
        for direction in range(2):
            if carries(direction, step, ch):
                t = source(direction, step)
                arrived(block(ch, t), agrecv.at[t, ch])
                if step < half:
                    forward(step + 1, ch, direction)

    def gather_step(step):
        gather_meta(step)
        for ch in range(NCH):
            gather_chunk(step, ch)

    for direction in range(2):
        forward_meta(1, direction)
    for ch in range(NCH):
        for direction in range(2):
            forward(1, ch, direction)
    for dx in (2, 1, 3):
        there = (nx - dx) % nx
        send(
            slab.at[0:rows, :],
            slab.at[there * rows : (there + 1) * rows, :],
            nsend.at[dx],
            nrecv.at[there],
            at(z, c, (x + dx) % nx),
        )

    def shared_expert():
        for dx in range(1, nx):
            arrived(slab.at[dx * rows : (dx + 1) * rows, :], nrecv.at[dx])
        load_sg.wait()
        load_su.wait()
        load_sd.wait()
        both = dot(slab[...], wsh[...])
        hidden = (silu(both[:, 0:unit]) * both[:, unit : 2 * unit]).astype(BF16)
        for ch in range(NCH):
            cols = slice(ch * cw, (ch + 1) * cw)
            shp[:, cols] = dot(hidden, sd[:, cols]).astype(BF16)

    def shared_out():
        for dx in (2, 1, 3):
            there = (nx - dx) % nx
            send(
                shp.at[dx * rows : (dx + 1) * rows, :],
                shr.at[there],
                ssend.at[dx],
                srecv.at[there],
                at(z, c, (x + dx) % nx),
            )

    def build(g):
        lane8 = iota((8, 128), 1)
        seg8 = lane8 // rows
        codes, gws = [], []
        for v in range(2):
            code = jnp.full((8, 128), -4.0, F32)
            gate = jnp.zeros((8, 128), F32)
            for i in range(4):
                p = 4 * v + i
                if p > PER:
                    continue
                tile = meta[0 if p == 0 else PER * g + p]
                ahead = pltpu.roll(tile, i * rows, 1) if i > 0 else tile
                code = jnp.where(seg8 == i, ahead, code)
                ahead = pltpu.roll(tile, (i + 3) % 4 * rows, 1) if i != 1 else tile
                gate = jnp.where(seg8 == i, ahead, gate)
            codes.append(code)
            gws.append(gate)
        rr = iota((group_rows, 128), 0)
        bi = (rr * 11) >> 5
        last = rr == group_rows - 1
        pos_r = jnp.where(last, 0, 1 + bi)
        rank_r = jnp.where(last, g, rr - 3 * bi)
        seg = iota((group_rows, 128), 1) // rows
        turned = []
        for q in range(plane):
            cq, xq = mate(q)
            expert = plane * z + nx * cq + xq
            want = (rank_r + 4 * expert).astype(F32)
            lines = []
            for v in range(2):
                placed = pos_r == seg + 4 * v
                one = jnp.zeros((group_rows, 128), F32)
                weight = jnp.zeros((group_rows, 128), F32)
                for k in range(TOPK):
                    match = (codes[v][k : k + 1, :] == want) & placed
                    one = jnp.where(match, 1.0, one)
                    weight = jnp.where(match, gws[v][k : k + 1, :], weight)
                sel[g, q * group_rows : (q + 1) * group_rows, v * 128 : (v + 1) * 128] = one.astype(
                    BF16
                )
                lines.append(weight)
            turned.append(lines)
        for v in range(2):
            column = jnp.concatenate([turned[q][v] for q in range(plane)], axis=0)
            com[g, v * 128 : (v + 1) * 128, :] = column.T.astype(BF16)

    far = [2, nx + 2, 1, nx + 1, 3, nx + 3, nx]
    final = groups - 1

    def part_of(q):
        return slice(q * group_rows, (q + 1) * group_rows)

    def columns(ch):
        return slice(ch * cw, (ch + 1) * cw)

    def swap(g, ch, src, dst, ss, rs, ss2, rs2):
        for q in far:
            cq, xq = mate(q)
            b = back(q)
            if ch is None:
                send(
                    src.at[g, :, part_of(q), :],
                    dst.at[g, :, part_of(b), :],
                    ss.at[g, q],
                    rs.at[g, b],
                    at(z, cq, xq),
                )
            else:
                send(
                    src.at[g, ch, part_of(q), :],
                    dst.at[g, ch, part_of(b), :],
                    ss2.at[ch, q],
                    rs2.at[ch, b],
                    at(z, cq, xq),
                )

    def came(g, ch, dst, rs, rs2):
        for q in range(1, plane):
            if g < final:
                arrived(dst.at[g, :, part_of(q), :], rs.at[g, q])
            else:
                arrived(dst.at[g, ch, part_of(q), :], rs2.at[ch, q])

    def pick(g, ch):
        first = ag[ch, 0:rows, :]
        begin = (1 + PER * g) * rows
        stack = jnp.concatenate(
            [first, ag[ch, begin : begin + PER * rows, :], first, first], axis=0
        )
        picked = dot(sel[g], stack).astype(BF16)
        rb[g, ch, 0:group_rows, :] = picked[0:group_rows]
        sb[g, ch, group_rows:, :] = picked[group_rows:]

    def dispatch(g):
        build(g)
        for ch in range(NCH):
            pick(g, ch)
        swap(g, None, sb, rb, dsend, drecv, dsend2, drecv2)

    def enter(g, ch):
        rows_in = rb[g, ch]
        gate = dot(rows_in, eg[columns(ch), :])
        up = dot(rows_in, eu[columns(ch), :])
        if ch == 0:
            acc[0] = gate
            acc[1] = up
        else:
            acc[0] = acc[0] + gate
            acc[1] = acc[1] + up

    def leave(g, ch, hidden):
        made = dot(hidden, ed[:, columns(ch)]).astype(BF16)
        cb[g, ch, 0:group_rows, :] = made[0:group_rows]
        eo[g, ch, group_rows:, :] = made[group_rows:]

    def experts(g):
        came(g, None, rb, drecv, drecv2)
        taken = [rb[g, ch] for ch in range(NCH)]
        taken = jnp.concatenate(taken, axis=1)
        hidden = (silu(dot(taken, eg[...])) * dot(taken, eu[...])).astype(BF16)
        for ch in range(NCH):
            leave(g, ch, hidden)

    def give_back(g, ch):
        swap(g, ch, eo, cb, csend, crecv, csend2, crecv2)

    def combine(g, ch):
        used = (PER + 1) * rows
        summed = dot(com[g, 0:used, :], cb[g, ch])
        cols = columns(ch)
        if g == final:
            own[:, cols] = summed[0:rows]
        else:
            own[:, cols] = own[:, cols] + summed[0:rows]
        part[g * PER * rows : (g + 1) * PER * rows, cols] = summed[rows:used]

    def combine_all(g):
        came(g, None, cb, crecv, crecv2)
        for ch in range(NCH):
            combine(g, ch)

    gather_step(1)
    gather_step(2)
    gather_step(3)
    dispatch(0)
    gather_step(4)
    gather_step(5)
    dispatch(1)
    gather_step(6)
    load_eg.wait()
    load_eu.wait()
    load_ed.wait()
    experts(0)
    gather_step(7)
    gather_meta(8)
    build(final)
    for ch in range(NCH):
        gather_chunk(8, ch)
        pick(final, ch)
        swap(final, ch, sb, rb, dsend, drecv, dsend2, drecv2)
    experts(1)
    shared_expert()
    for ch in range(NCH):
        came(final, ch, rb, drecv, drecv2)
        enter(final, ch)
    hidden = (silu(acc[0]) * acc[1]).astype(BF16)
    for ch in range(NCH):
        leave(final, ch, hidden)
        give_back(final, ch)
    give_back(1, None)
    give_back(0, None)
    shared_out()

    def brings(direction, step, ch):
        return step > 1 or (ch < NCH // 2) == (direction == 0)

    def reduce_chunk(step, ch):
        distance = half + 1 - step
        for direction in range(2):
            if not brings(direction, step, ch):
                continue
            s = slot[distance if direction == 0 else -distance]
            value = part[(s - 1) * rows : s * rows, columns(ch)]
            if step > 1 and brings(direction, step - 1, ch):
                arrived(rsr.at[direction, step - 2, ch], rrecv.at[direction, step - 2, ch])
                value = value + rsr[direction, step - 2, ch].astype(F32)
            rss[direction, step - 1, ch] = value.astype(BF16)
            send(
                rss.at[direction, step - 1, ch],
                rsr.at[direction, step - 1, ch],
                rsend.at[direction, step - 1, ch],
                rrecv.at[direction, step - 1, ch],
                at(zs[direction], c, x),
            )

    events = sorted(
        (step + LAG * ch, step, ch) for step in range(1, half + 1) for ch in range(NCH)
    )
    merged = []
    for _, step, ch in events:
        if step == 1:
            came(final, ch, cb, crecv, crecv2)
            combine(final, ch)
        for g, least in ((1, 4), (0, 6)):
            if step == least and g not in merged:
                combine_all(g)
                merged.append(g)
        reduce_chunk(step, ch)

    base = stream[...] + shp[0:rows, :].astype(F32)
    for dx in range(1, nx):
        arrived(shr.at[dx], srecv.at[dx])
        base = base + shr[dx].astype(F32)
    stream[...] = base + own[...]
    for ch in range(NCH):
        cols = slice(ch * cw, (ch + 1) * cw)
        value = stream[:, cols]
        for direction in range(2):
            arrived(rsr.at[direction, half - 1, ch], rrecv.at[direction, half - 1, ch])
            value = value + rsr[direction, half - 1, ch].astype(F32)
        staged[:, cols] = value.astype(BF16)
        load(staged.at[:, cols], out_ref.at[:, cols])
    for copy in sent:
        copy.wait_send()
    for copy in loads[-NCH:]:
        copy.wait()


def body(nz, nx, *args):
    (
        query_rows,
        key_rows,
        value_rows,
        sink_logit,
        out_weight,
        residual,
        norm_gain,
        routes,
        gate_weights,
        expert_gate,
        expert_up,
        expert_down,
        shared_gate,
        shared_up,
        shared_down,
    ) = args
    rows, width = residual.shape
    span = query_rows.shape[0]
    half = nz // 2
    plane = 2 * nx
    groups = (nz - 1) // PER
    group_rows = PER * CAP + 1
    cw = width // NCH
    ff = expert_gate.shape[2]
    unit = shared_gate.shape[1]
    dma = pltpu.SemaphoreType.DMA
    vm = pltpu.VMEM
    scratch = [
        pltpu.SMEM(sink_logit.shape, F32),
        vm((1, width), F32),
        vm((TOPK, rows), jnp.int32),
        vm((TOPK, rows), F32),
        vm((span, query_rows.shape[1]), BF16),
        vm((2, 3 * span, key_rows.shape[1]), BF16),
        vm(out_weight.shape, BF16),
        vm((rows, width), BF16),
        vm((width, ff), BF16),
        vm((width, ff), BF16),
        vm((ff, width), BF16),
        vm((width, 2 * unit), BF16),
        vm((unit, width), BF16),
        vm((span, query_rows.shape[1]), BF16),
        vm((span, width), BF16),
        vm((nx, rows, width), BF16),
        vm((rows, width), F32),
        vm((nx * rows, width), BF16),
        vm((nx * rows, width), BF16),
        vm((nx, rows, width), BF16),
        vm((NCH, nz * rows, cw), BF16),
        vm((nz, 8, 128), F32),
        vm((groups, plane * group_rows, 256), BF16),
        vm((groups, 256, plane * group_rows), BF16),
        vm((groups, NCH, plane * group_rows, cw), BF16),
        vm((groups, NCH, plane * group_rows, cw), BF16),
        vm((groups, NCH, plane * group_rows, cw), BF16),
        vm((groups, NCH, plane * group_rows, cw), BF16),
        vm((2, plane * group_rows, ff), F32),
        vm(((nz - 1) * rows, width), F32),
        vm((rows, width), F32),
        vm((rows, width), BF16),
        vm((2, half, NCH, rows, cw), BF16),
        vm((2, half, NCH, rows, cw), BF16),
        dma((15 + NCH,)),
        dma((2,)),
        dma((2,)),
        dma((nx,)),
        dma((nx,)),
        dma((nx,)),
        dma((nx,)),
        dma((nx,)),
        dma((nx,)),
        dma((2, half, NCH)),
        dma((nz, NCH)),
        dma((2, half)),
        dma((nz,)),
        dma((groups - 1, plane)),
        dma((groups - 1, plane)),
        dma((groups - 1, plane)),
        dma((groups - 1, plane)),
        dma((NCH, plane)),
        dma((NCH, plane)),
        dma((NCH, plane)),
        dma((NCH, plane)),
        dma((2, half, NCH)),
        dma((2, half, NCH)),
    ]
    hbm = pl.BlockSpec(memory_space=pl.ANY)
    return pl.pallas_call(
        functools.partial(kernel, nz, nx),
        out_shape=jax.ShapeDtypeStruct((rows, width), BF16),
        in_specs=[hbm] * 15,
        out_specs=hbm,
        scratch_shapes=scratch,
        compiler_params=pltpu.CompilerParams(
            collective_id=0, has_side_effects=True, vmem_limit_bytes=60 * 1024 * 1024
        ),
    )(
        query_rows,
        key_rows,
        value_rows,
        sink_logit,
        out_weight,
        residual,
        norm_gain.reshape(1, width),
        routes.T,
        gate_weights.T,
        expert_gate,
        expert_up,
        expert_down,
        shared_gate,
        shared_up,
        shared_down,
    )


def solution(mesh):
    placed = (
        P(("grp", "sp"), "tp"),
        P(("grp", "sp"), "tp"),
        P(("grp", "sp"), "tp"),
        P("tp"),
        P("tp", None),
        P(("grp", "sp", "tp"), None),
        P(),
        P(("grp", "sp", "tp"), None),
        P(("grp", "sp", "tp"), None),
        P(("sp", "tp"), None, None),
        P(("sp", "tp"), None, None),
        P(("sp", "tp"), None, None),
        P(None, "tp"),
        P(None, "tp"),
        P("tp", None),
    )
    return jax.shard_map(
        functools.partial(body, mesh.shape["sp"] // 2, mesh.shape["tp"]),
        mesh=mesh,
        in_specs=placed,
        out_specs=P(("grp", "sp", "tp"), None),
        check_vma=False,
    )
```
